32 devices in a mesh: sp: 8 (over z, y), tp: 4 (over x, core).
Axes of the slice: x: 2, y: 2, z: 4, core: 2. Of those that a mesh axis runs over, the one named last changes fastest.
Arguments:
- mix_input: bfloat16 [2048, 1024], P('sp', 'tp'), may hold values from -6 to 6
- stream: bfloat16 [2048, 2048], P(('sp', 'tp')), may hold values from -48 to 48
- doc_ids: int32 [2048], P('sp'), may hold values from 0 to 3, never falling along the last dimension, each value on 1 to 1024 neighbouring positions
- log_dt: float32 [64], P('tp'), may hold values from -12 to -2
- decay_rate: float32 [64, 64], P('tp'), may hold values from 0.5 to 1
- frequency: float32 [64, 64], P('tp'), may hold values from 0 to 64
- input_real: float32 [2, 64, 64, 16], P(None, 'tp'), may hold values from -400 to 400
- input_imag: float32 [2, 64, 64, 16], P(None, 'tp'), may hold values from -400 to 400
- output_real: float32 [2, 64, 16, 64], P(None, 'tp'), may hold values from -0.75 to 0.75
- output_imag: float32 [2, 64, 16, 64], P(None, 'tp'), may hold values from -0.75 to 0.75
- skip_gain: float32 [1024], P('tp'), may hold values from -4 to 4
- log_keep: float32 [64, 2048], P('tp', 'sp'), may hold values from -2 to 0
- proj_weight: bfloat16 [1024, 2048], P('tp'), may hold values from -0.1875 to 0.1875
- norm_gain: float32 [2048], replicated, may hold values from 0.1 to 1.9
- gate_weight: bfloat16 [2048, 5632], P('sp', 'tp'), may hold values from -0.125 to 0.125
- up_weight: bfloat16 [2048, 5632], P('sp', 'tp'), may hold values from -0.125 to 0.125
- down_weight: bfloat16 [5632, 2048], P('tp', 'sp'), may hold values from -0.078125 to 0.078125
Outputs:
- layer_out: bfloat16 [2048, 2048], P(('sp', 'tp'))
The draws below stay inside these ranges and needn't reach their ends.
Inputs may be any that keep to these rules, and one draw needn't show every extreme that they name: `doc_ids`: document numbers never fall along the positions; a document covers at most half of the positions.
All inputs are finite; a program needn't handle non-finite values.
Results may differ from the reference program's by a relative error of at most 0.009.
Values may be sent and summed in bfloat16 or wider, within the bound.
A program may use at most 128 MiB of HBM per device.

```python
import math
import jax
import jax.numpy as jnp
import numpy as np
from jax import lax

D = 2048
WIDTH = 1024
GROUP = 16
STATE = 64
FF = 5632
TOK_DEV = 256
DOCS = 4
GROUPS = 64
TOKENS = 2048
N_TP = 4


def group_steps(key):
    base = jax.random.fold_in(key, 11)
    first_key, second_key, third_key = jax.random.split(base, 3)
    picked = jax.random.uniform(first_key, (GROUPS,), jnp.float32)
    slower = picked < 0.5
    slow_value = math.log(0.5 / TOKENS) + jax.random.uniform(second_key, (GROUPS,), jnp.float32, -0.3, 0.3)
    fast_value = jax.random.uniform(third_key, (GROUPS,), jnp.float32, math.log(0.04), math.log(0.05))
    return jnp.where(slower, slow_value, fast_value)


def draw_log_dt(key, part):
    return group_steps(key).astype(jnp.float32)


def input_matrix(key, salt):
    log_step = group_steps(key)
    scale = jnp.sqrt(2.0 / (jnp.exp(log_step) * GROUP))
    noise = jax.random.truncated_normal(jax.random.fold_in(key, salt), -4.0, 4.0, (2, GROUPS, STATE, GROUP), jnp.float32)
    return (noise * scale[None, :, None, None]).astype(jnp.float32)


def draw_input_real(key, part):
    return input_matrix(key, 21)


def draw_input_imag(key, part):
    return input_matrix(key, 22)


def draw_log_keep(key, part):
    base = jax.random.fold_in(key, 31)
    first_key, second_key, third_key, fourth_random_key = jax.random.split(base, 4)
    blocks = TOKENS // TOK_DEV
    level = jnp.exp(jax.random.uniform(first_key, (GROUPS, blocks), jnp.float32, math.log(0.1), 0.0)) / TOKENS
    per_slot_feedforward = jnp.repeat(level, TOK_DEV, axis=1) * jax.random.uniform(second_key, (GROUPS, TOKENS), jnp.float32, 0.0, 2.0)
    slot_indices = jax.random.randint(third_key, (GROUPS, 2), 0, TOKENS)
    stack_level_count = jax.random.uniform(fourth_random_key, (GROUPS, 2), jnp.float32, 0.22, 0.69)
    sequence_offsets = jnp.arange(TOKENS, dtype=jnp.int32)
    segment_sets = jnp.sum((sequence_offsets[None, None, :] == slot_indices[:, :, None]).astype(jnp.float32) * stack_level_count[:, :, None], axis=1)
    return (-(per_slot_feedforward + segment_sets)).astype(jnp.float32)


def draw_stream(key, part):
    base = jax.random.fold_in(key, 41)
    first_key, second_key, third_key = jax.random.split(base, 3)
    row_scale = jnp.exp(jax.random.uniform(first_key, (TOKENS, 1), jnp.float32, math.log(0.3), math.log(3.0)))
    col_scale = jnp.exp(jax.random.uniform(second_key, (1, D), jnp.float32, math.log(0.3), math.log(3.0)))
    values = jax.random.truncated_normal(third_key, -4.0, 4.0, (TOKENS, D), jnp.float32)
    return (values * row_scale * col_scale).astype(jnp.bfloat16)


def block_levels(own_key, extent, shards, least, largest):
    level = 1.0
    for axis_at, parts in shards:
        draws = jax.random.uniform(jax.random.fold_in(jax.random.fold_in(own_key, 6), axis_at), (parts,), jnp.float32, least / len(shards), largest / len(shards))
        level = level * jnp.repeat(jnp.exp(draws), extent[axis_at] // parts).reshape((-1,) + (1,) * (len(extent) - 1 - axis_at))
    return level


def split_up(amount, total, reach, slope):
    loads = [(1 << 20) // math.isqrt(rank ** slope) + 1 for rank in range(2, amount + 1)]
    surplus, holding = total - reach - (amount - 1), [1] * (amount - 1)
    while surplus > 0:
        candidates = [i for i in range(amount - 1) if holding[i] < reach]
        mass, left = sum([loads[i] for i in candidates]), surplus
        for i in candidates:
            extra = min(reach - holding[i], max(1, left * loads[i] // mass), surplus)
            holding[i] = holding[i] + extra
            surplus = surplus - extra
    return np.array([reach] + holding)


def uneven(rng, count, total, most, lean):
    if count == 2:
        one = jax.random.randint(rng, (), max(1, total - most), min(most, total - 1) + 1)
        return jnp.stack([one, total - one])
    sizes = jnp.asarray(split_up(count, total, most, lean), jnp.int32)
    couples = (count - 1) // 2
    giver, receiver = sizes[1:1 + 2 * couples:2], sizes[2:2 + 2 * couples:2]
    room = jnp.minimum(giver - 1, most - receiver)
    moved = jax.random.randint(jax.random.fold_in(rng, 1), (couples,), 0, 1 << 20) % (room + 1)
    sizes = sizes.at[1:1 + 2 * couples:2].set(giver - moved).at[2:2 + 2 * couples:2].set(receiver + moved)
    return sizes[jax.random.permutation(jax.random.fold_in(rng, 2), count)]


def scatter_about(stream_key, shape, scale, bound, cuts=(), kind=jnp.bfloat16):
    array = scale * jax.random.normal(stream_key, shape, jnp.float32)
    if cuts:
        array = array * block_levels(stream_key, shape, cuts, -0.22, 0.18)
    return jnp.clip(array, -bound, bound).astype(kind)


def setup_inputs(seed: int = 0) -> dict:
    streams_of = jax.random.split(jax.random.key(seed), 18)
    return {
        "mix_input": scatter_about(streams_of[0], (TOKENS, WIDTH), 1.0, 6.0, ((0, 8), (1, 4))),
        "stream": draw_stream(jax.random.fold_in(streams_of[17], 71), 0),
        "doc_ids": jnp.searchsorted(jnp.cumsum(uneven(streams_of[2], DOCS, TOKENS, TOKENS // 2, 0)), jnp.arange(TOKENS), side="right").astype(jnp.int32),
        "log_dt": draw_log_dt(jax.random.fold_in(streams_of[17], 71), 0),
        "decay_rate": jnp.clip(jnp.exp(math.log(1.0) - 0.6931472 * jax.random.uniform(streams_of[4], (GROUPS, STATE), jnp.float32) ** block_levels(streams_of[4], (GROUPS, STATE), ((0, 4),), -0.2, 0.2)), 0.5, 1.0),
        "frequency": jnp.clip(64.0 * jax.random.uniform(streams_of[5], (GROUPS, STATE), jnp.float32) ** block_levels(streams_of[5], (GROUPS, STATE), ((0, 4),), -0.2, 0.2), 0.0, 64.0),
        "input_real": draw_input_real(jax.random.fold_in(streams_of[17], 71), 0),
        "input_imag": draw_input_imag(jax.random.fold_in(streams_of[17], 71), 0),
        "output_real": scatter_about(streams_of[8], (2, GROUPS, GROUP, STATE), STATE ** -0.5, 0.75, ((1, 4),), jnp.float32),
        "output_imag": scatter_about(streams_of[9], (2, GROUPS, GROUP, STATE), STATE ** -0.5, 0.75, ((1, 4),), jnp.float32),
        "skip_gain": scatter_about(streams_of[10], (WIDTH,), 1.0, 4.0, ((0, 4),), jnp.float32),
        "log_keep": draw_log_keep(jax.random.fold_in(streams_of[17], 71), 0),
        "proj_weight": scatter_about(streams_of[12], (WIDTH, D), WIDTH ** -0.5, 0.1875, ((0, 4),)),
        "norm_gain": jnp.clip(1.0 + 0.18 * jax.random.normal(streams_of[13], (D,), jnp.float32), 0.1, 1.9),
        "gate_weight": scatter_about(streams_of[14], (D, FF), D ** -0.5, 0.125, ((0, 8), (1, 4))),
        "up_weight": scatter_about(streams_of[15], (D, FF), D ** -0.5, 0.125, ((0, 8), (1, 4))),
        "down_weight": scatter_about(streams_of[16], (FF, D), FF ** -0.5, 0.078125, ((0, 4), (1, 8))),
    }


HIGHEST = lax.Precision.HIGHEST

def discretize(log_dt, decay_rate, frequency):
    step_size = jnp.exp(log_dt)[:, None]
    magnitude = jnp.exp(-step_size * decay_rate)
    angle_step = step_size * frequency
    state_real = magnitude * jnp.cos(angle_step)
    state_imag = magnitude * jnp.sin(angle_step)
    denominator = decay_rate * decay_rate + frequency * frequency
    shifted = state_real - 1.0
    zoh_real = (-shifted * decay_rate + state_imag * frequency) / denominator
    holdfixed_angle_part = (-state_imag * decay_rate - shifted * frequency) / denominator
    return (state_real, state_imag, zoh_real, holdfixed_angle_part)

def input_maps(zoh_real, holdfixed_angle_part, input_real, input_imag):
    scale_real = zoh_real[None, :, :, None]
    scale_imag = holdfixed_angle_part[None, :, :, None]
    return (scale_real * input_real - scale_imag * input_imag, scale_real * input_imag + scale_imag * input_real)

def pair_combine(earlier, later):
    mult_one_real, mult_one_imag, first_state_real, state_one_imag = earlier
    mult_two_real, second_multiplier_imag, state_two_real, state_two_imag = later
    return (mult_two_real * mult_one_real - second_multiplier_imag * mult_one_imag, mult_two_real * mult_one_imag + second_multiplier_imag * mult_one_real, mult_two_real * first_state_real - second_multiplier_imag * state_one_imag + state_two_real, mult_two_real * state_one_imag + second_multiplier_imag * first_state_real + state_two_imag)

def rounded_sum(activations, weights, pieces):
    block_width = activations.shape[1] // pieces
    summed = jnp.zeros((activations.shape[0], weights.shape[1]), jnp.float32)
    for number in range(pieces):
        lower = number * block_width
        partial_value = jnp.dot(activations[:, lower:lower + block_width], weights[lower:lower + block_width], preferred_element_type=jnp.float32).astype(jnp.bfloat16)
        summed = summed + lax.optimization_barrier(partial_value).astype(jnp.float32)
    return summed

def reference(mix_input, stream, doc_ids, log_dt, decay_rate, frequency, input_real, input_imag, output_real, output_imag, skip_gain, log_keep, proj_weight, norm_gain, gate_weight, up_weight, down_weight):
    state_real, state_imag, zoh_real, holdfixed_angle_part = discretize(log_dt, decay_rate, frequency)
    map_real, map_imag = input_maps(zoh_real, holdfixed_angle_part, input_real, input_imag)
    channels = mix_input.astype(jnp.float32)
    grouped = channels.reshape(TOKENS, GROUPS, GROUP).transpose(1, 0, 2)
    same_doc = (doc_ids[1:] == doc_ids[:-1]).astype(jnp.float32)
    nothing = jnp.zeros((1,), jnp.float32)
    link_prev = jnp.concatenate([nothing, same_doc])
    link_next = jnp.concatenate([same_doc, nothing])
    keep_rates = jnp.exp(log_keep)

    def group_pass(packed):
        cluster_source, group_real, group_imag, group_map_real, group_map_imag, read_real, read_imag, keep_row = packed
        result = jnp.zeros((TOKENS, GROUP), jnp.float32)
        for direction, doc_links, reverse in ((0, link_prev, False), (1, link_next, True)):
            factor = (keep_row * doc_links)[:, None]
            mult_real = factor * group_real[None, :]
            mult_imag = factor * group_imag[None, :]
            drive_real = jnp.dot(cluster_source, group_map_real[direction].T, precision=HIGHEST)
            drive_imag = jnp.dot(cluster_source, group_map_imag[direction].T, precision=HIGHEST)
            scanned = lax.associative_scan(pair_combine, (mult_real, mult_imag, drive_real, drive_imag), reverse=reverse, axis=0)
            result = result + jnp.dot(scanned[2], read_real[direction].T, precision=HIGHEST)
            result = result - jnp.dot(scanned[3], read_imag[direction].T, precision=HIGHEST)
        return result
    outputs = lax.map(group_pass, (grouped, state_real, state_imag, map_real.transpose(1, 0, 2, 3), map_imag.transpose(1, 0, 2, 3), output_real.transpose(1, 0, 2, 3), output_imag.transpose(1, 0, 2, 3), keep_rates))
    mixed_pre = outputs.transpose(1, 0, 2).reshape(TOKENS, WIDTH) + skip_gain * channels
    mixed = jax.nn.gelu(mixed_pre).astype(jnp.bfloat16)
    branch = rounded_sum(mixed, proj_weight, N_TP)
    resid = stream.astype(jnp.float32) + branch
    scale = lax.rsqrt(lax.optimization_barrier(jnp.mean(resid * resid, axis=-1, keepdims=True)) + 1e-06)
    normed = (resid * scale * norm_gain).astype(jnp.bfloat16)
    block_width = FF // N_TP
    ffn = jnp.zeros((TOKENS, D), jnp.float32)
    for number in range(N_TP):
        lower = number * block_width
        gate = jnp.dot(normed, gate_weight[:, lower:lower + block_width], preferred_element_type=jnp.float32)
        upward = jnp.dot(normed, up_weight[:, lower:lower + block_width], preferred_element_type=jnp.float32)
        hidden = (jax.nn.silu(gate) * upward).astype(jnp.bfloat16)
        partial_value = jnp.dot(hidden, down_weight[lower:lower + block_width], preferred_element_type=jnp.float32).astype(jnp.bfloat16)
        ffn = ffn + lax.optimization_barrier(partial_value).astype(jnp.float32)
    return (resid + 0.5 * ffn).astype(jnp.bfloat16)
```

```python
import functools

import jax
import jax.numpy as jnp
from jax import lax
from jax.experimental import pallas as pl
from jax.experimental.pallas import tpu as pltpu
from jax.sharding import PartitionSpec as P

GROUP = 16
CHUNKS = 8
BF = jnp.bfloat16
F32 = jnp.float32


def discretize(log_dt, decay_rate, frequency):
    step_size = jnp.exp(log_dt)[:, None]
    magnitude = jnp.exp(-step_size * decay_rate)
    angle_step = step_size * frequency
    state_real = magnitude * jnp.cos(angle_step)
    state_imag = magnitude * jnp.sin(angle_step)
    denominator = decay_rate * decay_rate + frequency * frequency
    shifted = state_real - 1.0
    zoh_real = (-shifted * decay_rate + state_imag * frequency) / denominator
    holdfixed_angle_part = (-state_imag * decay_rate - shifted * frequency) / denominator
    return (state_real, state_imag, zoh_real, holdfixed_angle_part)


def input_maps(zoh_real, holdfixed_angle_part, input_real, input_imag):
    scale_real = zoh_real[None, :, :, None]
    scale_imag = holdfixed_angle_part[None, :, :, None]
    return (
        scale_real * input_real - scale_imag * input_imag,
        scale_real * input_imag + scale_imag * input_real,
    )


def split(value):
    high = value.astype(BF)
    return high, (value - high.astype(F32)).astype(BF)


def dot_nt(left, right):
    return lax.dot_general(left, right, (((1,), (1,)), ((), ())), preferred_element_type=F32)


def one_hot(shape, row_of, lane_of):
    rows = lax.broadcasted_iota(jnp.int32, shape, 0)
    lanes = lax.broadcasted_iota(jnp.int32, shape, 1)
    return row_of(rows) == lane_of(lanes)


def spread_keep(keep, groups, states):
    pick = one_hot((groups, groups * states), lambda r: r, lambda c: c // states)
    pick = pick.astype(F32).astype(BF)
    first, rest = split(keep)
    rest32 = keep - first.astype(F32)
    second, third = split(rest32)
    return (
        jnp.dot(first, pick, preferred_element_type=F32)
        + jnp.dot(second, pick, preferred_element_type=F32)
        + jnp.dot(third, pick, preferred_element_type=F32)
    )


def cmul(ar, ai, br, bi):
    return ar * br - ai * bi, ar * bi + ai * br


def power(real, imag, count):
    result = None
    while count:
        if count & 1:
            result = (real, imag) if result is None else cmul(*result, real, imag)
        count >>= 1
        if count:
            real, imag = cmul(real, imag, real, imag)
    return result


def drive_kernel(
    u_ref, keep_ref, map_ref, pole_ref, doc_ref, drive_ref, chunk_ref, total_ref, factor_ref
):
    tokens, width = u_ref.shape
    flat = pole_ref.shape[1]
    groups = width // GROUP
    states = flat // groups
    span = tokens // CHUNKS
    u = u_ref[...]
    tile = one_hot((GROUP, width), lambda r: r, lambda c: c % GROUP).astype(F32).astype(BF)
    own = one_hot((flat, width), lambda r: r // states, lambda c: c // GROUP)
    for quarter in range(4):
        total = None
        for piece in split(map_ref[quarter]):
            wide = jnp.dot(piece, tile, preferred_element_type=F32)
            wide = jnp.where(own, wide, 0.0).astype(BF)
            part = dot_nt(u, wide)
            total = part if total is None else total + part
        drive_ref[quarter] = total
    pole_real = jnp.broadcast_to(pole_ref[0:1], (CHUNKS, flat))
    pole_imag = jnp.broadcast_to(pole_ref[1:2], (CHUNKS, flat))
    long_real, long_imag = power(pole_ref[0:1], pole_ref[1:2], span)
    for way in range(2):
        factor_ref[...] = spread_keep(keep_ref[way], groups, states)

        def step(k, carry):
            real, imag, kept = carry
            at = k if way == 0 else span - 1 - k
            rows = pl.ds(pl.multiple_of(at * CHUNKS, CHUNKS), CHUNKS)
            factor = factor_ref[rows]
            real, imag = factor * real, factor * imag
            real, imag = cmul(pole_real, pole_imag, real, imag)
            return (
                real + drive_ref[2 * way, rows],
                imag + drive_ref[2 * way + 1, rows],
                kept * factor,
            )

        zero = jnp.zeros((CHUNKS, flat), F32)
        real, imag, kept = lax.fori_loop(0, span, step, (zero, zero, zero + 1.0))
        mult_real, mult_imag = kept * long_real, kept * long_imag
        for number, item in enumerate((mult_real, mult_imag, real, imag)):
            chunk_ref[way, number] = item
        state = (jnp.zeros((1, flat), F32), jnp.zeros((1, flat), F32))
        product = (jnp.ones((1, flat), F32), jnp.zeros((1, flat), F32))
        for chunk in range(CHUNKS) if way == 0 else range(CHUNKS - 1, -1, -1):
            here = [chunk_ref[way, number, chunk : chunk + 1] for number in range(4)]
            product = cmul(here[0], here[1], *product)
            moved = cmul(here[0], here[1], *state)
            state = (moved[0] + here[2], moved[1] + here[3])
        for number, item in enumerate(product + state):
            total_ref[4 * way + number : 4 * way + number + 1] = item
    total_ref[8:9] = jnp.full((1, flat), doc_ref[0], F32)
    total_ref[9:10] = jnp.full((1, flat), doc_ref[1], F32)
    total_ref[10:16] = jnp.zeros((6, flat), F32)


def read_kernel(
    devices,
    u_ref,
    keep_ref,
    drive_ref,
    chunk_ref,
    all_ref,
    read_ref,
    pole_ref,
    skip_ref,
    doc_ref,
    me_ref,
    out_ref,
    factor_ref,
    start_ref,
    real_ref,
    imag_ref,
    y_ref,
):
    tokens, width = u_ref.shape
    flat = pole_ref.shape[1]
    groups = width // GROUP
    states = flat // groups
    span = tokens // CHUNKS
    me = me_ref[0]
    y_ref[...] = skip_ref[...] * u_ref[...].astype(F32)
    pole_real = jnp.broadcast_to(pole_ref[0:1], (CHUNKS, flat))
    pole_imag = jnp.broadcast_to(pole_ref[1:2], (CHUNKS, flat))
    tile = one_hot((states, flat), lambda r: r, lambda c: c % states).astype(F32).astype(BF)
    own = one_hot((width, flat), lambda r: r // GROUP, lambda c: c // states)
    for way in range(2):
        real = jnp.zeros((1, flat), F32)
        imag = jnp.zeros((1, flat), F32)
        edge = jnp.full((1, flat), -1.0, F32)
        for device in range(devices) if way == 0 else range(devices - 1, -1, -1):
            reached = jnp.full((1, flat), device, jnp.int32)
            reached = reached < me if way == 0 else reached > me
            row = [all_ref[device, 4 * way + k : 4 * way + k + 1] for k in range(4)]
            near = all_ref[device, 8 + way : 9 + way]
            far = all_ref[device, 9 - way : 10 - way]
            joined = jnp.where(near == edge, 1.0, 0.0)
            moved = cmul(row[0], row[1], joined * real, joined * imag)
            real = jnp.where(reached, moved[0] + row[2], real)
            imag = jnp.where(reached, moved[1] + row[3], imag)
            edge = jnp.where(reached, far, edge)
        joined = jnp.where(jnp.full((1, flat), doc_ref[way], F32) == edge, 1.0, 0.0)
        real, imag = joined * real, joined * imag
        for chunk in range(CHUNKS) if way == 0 else range(CHUNKS - 1, -1, -1):
            start_ref[0, chunk : chunk + 1] = real
            start_ref[1, chunk : chunk + 1] = imag
            here = [chunk_ref[way, number, chunk : chunk + 1] for number in range(4)]
            moved = cmul(here[0], here[1], real, imag)
            real, imag = moved[0] + here[2], moved[1] + here[3]
        factor_ref[...] = spread_keep(keep_ref[way], groups, states)

        def step(k, carry):
            real, imag = carry
            at = k if way == 0 else span - 1 - k
            rows = pl.ds(pl.multiple_of(at * CHUNKS, CHUNKS), CHUNKS)
            factor = factor_ref[rows]
            real, imag = factor * real, factor * imag
            real, imag = cmul(pole_real, pole_imag, real, imag)
            real = real + drive_ref[2 * way, rows]
            imag = imag + drive_ref[2 * way + 1, rows]
            real_ref[rows] = real
            imag_ref[rows] = imag
            return real, imag

        lax.fori_loop(0, span, step, (start_ref[0], start_ref[1]))
        for part, held in enumerate((real_ref, imag_ref)):
            high, low = split(held[...])
            read_high, read_low = split(read_ref[2 * way + part])
            wide_high = jnp.dot(read_high, tile, preferred_element_type=F32)
            wide_high = jnp.where(own, wide_high, 0.0).astype(BF)
            wide_low = jnp.dot(read_low, tile, preferred_element_type=F32)
            wide_low = jnp.where(own, wide_low, 0.0).astype(BF)
            y_ref[...] += (
                dot_nt(high, wide_high) + dot_nt(low, wide_high) + dot_nt(high, wide_low)
            )
    y = y_ref[...]
    inner = 0.7978845608028654 * (y + 0.044715 * (y * y * y))
    out_ref[...] = (0.5 * y * (1.0 + jnp.tanh(inner))).astype(BF)


def vmem(count):
    return [pl.BlockSpec(memory_space=pltpu.VMEM)] * count


def smem(count):
    return [pl.BlockSpec(memory_space=pltpu.SMEM)] * count


def interleave(array):
    tokens = array.shape[0]
    parts = array.reshape((CHUNKS, tokens // CHUNKS) + array.shape[1:])
    return jnp.swapaxes(parts, 0, 1).reshape(array.shape)


def deinterleave(array):
    tokens = array.shape[0]
    parts = array.reshape((tokens // CHUNKS, CHUNKS) + array.shape[1:])
    return jnp.swapaxes(parts, 0, 1).reshape(array.shape)


def mixing(
    mix_input, doc_ids, log_dt, decay_rate, frequency, input_real, input_imag,
    output_real, output_imag, skip_gain, log_keep,
):
    tokens, width = mix_input.shape
    groups, states = decay_rate.shape
    flat = groups * states
    pole_real, pole_imag, zoh_real, zoh_imag = discretize(log_dt, decay_rate, frequency)
    map_real, map_imag = input_maps(zoh_real, zoh_imag, input_real, input_imag)
    maps = jnp.stack([map_real, map_imag], 1).reshape(4, flat, GROUP)
    reads = jnp.stack([output_real, -output_imag], 1).reshape(4, width, states)
    poles = jnp.stack([pole_real.reshape(flat), pole_imag.reshape(flat)])
    same = (doc_ids[1:] == doc_ids[:-1]).astype(F32)
    one = jnp.ones((1,), F32)
    links = jnp.stack([jnp.concatenate([one, same]), jnp.concatenate([same, one])])
    keep = jnp.exp(log_keep).T[None] * links[:, :, None]
    keep = jnp.stack([interleave(keep[0]), interleave(keep[1])])
    u = interleave(mix_input)
    doc_edges = jnp.stack([doc_ids[0], doc_ids[-1]]).astype(F32)
    drive, chunk, total = pl.pallas_call(
        drive_kernel,
        out_shape=(
            jax.ShapeDtypeStruct((4, tokens, flat), F32),
            jax.ShapeDtypeStruct((2, 4, CHUNKS, flat), F32),
            jax.ShapeDtypeStruct((16, flat), F32),
        ),
        in_specs=vmem(4) + smem(1),
        out_specs=tuple(vmem(3)),
        scratch_shapes=[pltpu.VMEM((tokens, flat), F32)],
        compiler_params=pltpu.CompilerParams(vmem_limit_bytes=40 << 20),
        cost_estimate=pl.CostEstimate(flops=10**8, bytes_accessed=6 << 20, transcendentals=0),
        name="drive",
    )(u, keep, maps, poles, doc_edges)
    everything = lax.all_gather(total, "sp")
    devices = everything.shape[0]
    me = lax.axis_index("sp").astype(jnp.int32).reshape(1)
    mixed = pl.pallas_call(
        functools.partial(read_kernel, devices),
        out_shape=jax.ShapeDtypeStruct((tokens, width), BF),
        in_specs=vmem(8) + smem(2),
        out_specs=vmem(1)[0],
        scratch_shapes=[
            pltpu.VMEM((tokens, flat), F32),
            pltpu.VMEM((2, CHUNKS, flat), F32),
            pltpu.VMEM((tokens, flat), F32),
            pltpu.VMEM((tokens, flat), F32),
            pltpu.VMEM((tokens, width), F32),
        ],
        compiler_params=pltpu.CompilerParams(vmem_limit_bytes=40 << 20),
        cost_estimate=pl.CostEstimate(flops=10**8, bytes_accessed=6 << 20, transcendentals=0),
        name="read",
    )(u, keep, drive, chunk, everything, reads, poles, skip_gain[None], doc_edges, me)
    return deinterleave(mixed)


def rounded_sum(activations, weights, pieces):
    block_width = activations.shape[1] // pieces
    summed = jnp.zeros((activations.shape[0], weights.shape[1]), jnp.float32)
    for number in range(pieces):
        lower = number * block_width
        partial_value = jnp.dot(
            activations[:, lower : lower + block_width],
            weights[lower : lower + block_width],
            preferred_element_type=jnp.float32,
        ).astype(jnp.bfloat16)
        summed = summed + lax.optimization_barrier(partial_value).astype(jnp.float32)
    return summed


def local(
    mix_input,
    stream,
    doc_ids,
    log_dt,
    decay_rate,
    frequency,
    input_real,
    input_imag,
    output_real,
    output_imag,
    skip_gain,
    log_keep,
    proj_weight,
    norm_gain,
    gate_weight,
    up_weight,
    down_weight,
):
    mixed = mixing(
        mix_input, doc_ids, log_dt, decay_rate, frequency, input_real, input_imag,
        output_real, output_imag, skip_gain, log_keep,
    )
    tp_size = lax.axis_size("tp")
    spread = lax.all_to_all(mixed, "tp", split_axis=0, concat_axis=1, tiled=True)
    proj_whole = lax.all_gather(proj_weight, "tp", axis=0, tiled=True)
    branch = rounded_sum(spread, proj_whole, tp_size)
    resid = stream.astype(jnp.float32) + branch
    scale = lax.rsqrt(jnp.mean(resid * resid, axis=-1, keepdims=True) + 1e-06)
    normed = (resid * scale * norm_gain).astype(jnp.bfloat16)
    rows_all = lax.all_gather(normed, "tp", axis=0, tiled=True)
    gate = jnp.dot(
        rows_all,
        lax.all_gather(gate_weight, "sp", axis=0, tiled=True),
        preferred_element_type=jnp.float32,
    )
    upward = jnp.dot(
        rows_all,
        lax.all_gather(up_weight, "sp", axis=0, tiled=True),
        preferred_element_type=jnp.float32,
    )
    hidden = (jax.nn.silu(gate) * upward).astype(jnp.bfloat16)
    partial_out = jnp.dot(
        hidden,
        lax.all_gather(down_weight, "sp", axis=1, tiled=True),
        preferred_element_type=jnp.float32,
    )
    ffn = lax.psum_scatter(
        partial_out.astype(jnp.bfloat16), "tp", scatter_dimension=0, tiled=True
    ).astype(jnp.float32)
    return (resid + 0.5 * ffn).astype(jnp.bfloat16)


def solution(mesh):
    placed = (
        P("sp", "tp"),
        P(("sp", "tp"), None),
        P("sp"),
        P("tp"),
        P("tp", None),
        P("tp", None),
        P(None, "tp", None, None),
        P(None, "tp", None, None),
        P(None, "tp", None, None),
        P(None, "tp", None, None),
        P("tp"),
        P("tp", "sp"),
        P("tp", None),
        P(),
        P("sp", "tp"),
        P("sp", "tp"),
        P("tp", "sp"),
    )
    return jax.shard_map(
        local, mesh=mesh, in_specs=placed, out_specs=P(("sp", "tp"), None), check_vma=False
    )
```

```python
import functools

import jax
import jax.numpy as jnp
from jax import lax
from jax.experimental import pallas as pl
from jax.experimental.pallas import tpu as pltpu
from jax.sharding import PartitionSpec as P

GROUP = 16
CHUNKS = 8
BF = jnp.bfloat16
F32 = jnp.float32


def discretize(log_dt, decay_rate, frequency):
    step_size = jnp.exp(log_dt)[:, None]
    magnitude = jnp.exp(-step_size * decay_rate)
    angle_step = step_size * frequency
    state_real = magnitude * jnp.cos(angle_step)
    state_imag = magnitude * jnp.sin(angle_step)
    denominator = decay_rate * decay_rate + frequency * frequency
    shifted = state_real - 1.0
    zoh_real = (-shifted * decay_rate + state_imag * frequency) / denominator
    holdfixed_angle_part = (-state_imag * decay_rate - shifted * frequency) / denominator
    return (state_real, state_imag, zoh_real, holdfixed_angle_part)


def input_maps(zoh_real, holdfixed_angle_part, input_real, input_imag):
    scale_real = zoh_real[None, :, :, None]
    scale_imag = holdfixed_angle_part[None, :, :, None]
    return (
        scale_real * input_real - scale_imag * input_imag,
        scale_real * input_imag + scale_imag * input_real,
    )


def split(value):
    high = value.astype(BF)
    return high, (value - high.astype(F32)).astype(BF)


def dot_nt(left, right):
    return lax.dot_general(left, right, (((1,), (1,)), ((), ())), preferred_element_type=F32)


def one_hot(shape, row_of, lane_of):
    rows = lax.broadcasted_iota(jnp.int32, shape, 0)
    lanes = lax.broadcasted_iota(jnp.int32, shape, 1)
    return row_of(rows) == lane_of(lanes)


def spread_keep(keep, groups, states):
    pick = one_hot((groups, groups * states), lambda r: r, lambda c: c // states)
    pick = pick.astype(F32).astype(BF)
    first, rest = split(keep)
    rest32 = keep - first.astype(F32)
    second, third = split(rest32)
    return (
        jnp.dot(first, pick, preferred_element_type=F32)
        + jnp.dot(second, pick, preferred_element_type=F32)
        + jnp.dot(third, pick, preferred_element_type=F32)
    )


def cmul(ar, ai, br, bi):
    return ar * br - ai * bi, ar * bi + ai * br


def power(real, imag, count):
    result = None
    while count:
        if count & 1:
            result = (real, imag) if result is None else cmul(*result, real, imag)
        count >>= 1
        if count:
            real, imag = cmul(real, imag, real, imag)
    return result


def drive_kernel(
    u_ref, keep_ref, map_ref, pole_ref, doc_ref, drive_ref, chunk_ref, total_ref, factor_ref
):
    tokens, width = u_ref.shape
    flat = pole_ref.shape[1]
    groups = width // GROUP
    states = flat // groups
    span = tokens // CHUNKS
    u = u_ref[...]
    tile = one_hot((GROUP, width), lambda r: r, lambda c: c % GROUP).astype(F32).astype(BF)
    own = one_hot((flat, width), lambda r: r // states, lambda c: c // GROUP)
    for quarter in range(4):
        total = None
        for piece in split(map_ref[quarter]):
            wide = jnp.dot(piece, tile, preferred_element_type=F32)
            wide = jnp.where(own, wide, 0.0).astype(BF)
            part = dot_nt(u, wide)
            total = part if total is None else total + part
        drive_ref[quarter] = total
    pole_real = jnp.broadcast_to(pole_ref[0:1], (CHUNKS, flat))
    pole_imag = jnp.broadcast_to(pole_ref[1:2], (CHUNKS, flat))
    long_real, long_imag = power(pole_ref[0:1], pole_ref[1:2], span)
    for way in range(2):
        factor_ref[...] = spread_keep(keep_ref[way], groups, states)

        def step(k, carry):
            real, imag, kept = carry
            at = k if way == 0 else span - 1 - k
            rows = pl.ds(pl.multiple_of(at * CHUNKS, CHUNKS), CHUNKS)
            factor = factor_ref[rows]
            real, imag = factor * real, factor * imag
            real, imag = cmul(pole_real, pole_imag, real, imag)
            return (
                real + drive_ref[2 * way, rows],
                imag + drive_ref[2 * way + 1, rows],
                kept * factor,
            )

        zero = jnp.zeros((CHUNKS, flat), F32)
        real, imag, kept = lax.fori_loop(0, span, step, (zero, zero, zero + 1.0))
        mult_real, mult_imag = kept * long_real, kept * long_imag
        for number, item in enumerate((mult_real, mult_imag, real, imag)):
            chunk_ref[way, number] = item
        state = (jnp.zeros((1, flat), F32), jnp.zeros((1, flat), F32))
        product = (jnp.ones((1, flat), F32), jnp.zeros((1, flat), F32))
        for chunk in range(CHUNKS) if way == 0 else range(CHUNKS - 1, -1, -1):
            here = [chunk_ref[way, number, chunk : chunk + 1] for number in range(4)]
            product = cmul(here[0], here[1], *product)
            moved = cmul(here[0], here[1], *state)
            state = (moved[0] + here[2], moved[1] + here[3])
        for number, item in enumerate(product + state):
            total_ref[4 * way + number : 4 * way + number + 1] = item
    total_ref[8:9] = jnp.full((1, flat), doc_ref[0], F32)
    total_ref[9:10] = jnp.full((1, flat), doc_ref[1], F32)
    total_ref[10:16] = jnp.zeros((6, flat), F32)


def read_kernel(
    devices,
    u_ref,
    keep_ref,
    drive_ref,
    chunk_ref,
    all_ref,
    read_ref,
    pole_ref,
    skip_ref,
    doc_ref,
    me_ref,
    out_ref,
    factor_ref,
    start_ref,
    real_ref,
    imag_ref,
    y_ref,
):
    tokens, width = u_ref.shape
    flat = pole_ref.shape[1]
    groups = width // GROUP
    states = flat // groups
    span = tokens // CHUNKS
    me = me_ref[0]
    y_ref[...] = skip_ref[...] * u_ref[...].astype(F32)
    pole_real = jnp.broadcast_to(pole_ref[0:1], (CHUNKS, flat))
    pole_imag = jnp.broadcast_to(pole_ref[1:2], (CHUNKS, flat))
    tile = one_hot((states, flat), lambda r: r, lambda c: c % states).astype(F32).astype(BF)
    own = one_hot((width, flat), lambda r: r // GROUP, lambda c: c // states)
    for way in range(2):
        real = jnp.zeros((1, flat), F32)
        imag = jnp.zeros((1, flat), F32)
        edge = jnp.full((1, flat), -1.0, F32)
        for device in range(devices) if way == 0 else range(devices - 1, -1, -1):
            reached = jnp.full((1, flat), device, jnp.int32)
            reached = reached < me if way == 0 else reached > me
            row = [all_ref[device, 4 * way + k : 4 * way + k + 1] for k in range(4)]
            near = all_ref[device, 8 + way : 9 + way]
            far = all_ref[device, 9 - way : 10 - way]
            joined = jnp.where(near == edge, 1.0, 0.0)
            moved = cmul(row[0], row[1], joined * real, joined * imag)
            real = jnp.where(reached, moved[0] + row[2], real)
            imag = jnp.where(reached, moved[1] + row[3], imag)
            edge = jnp.where(reached, far, edge)
        joined = jnp.where(jnp.full((1, flat), doc_ref[way], F32) == edge, 1.0, 0.0)
        real, imag = joined * real, joined * imag
        for chunk in range(CHUNKS) if way == 0 else range(CHUNKS - 1, -1, -1):
            start_ref[0, chunk : chunk + 1] = real
            start_ref[1, chunk : chunk + 1] = imag
            here = [chunk_ref[way, number, chunk : chunk + 1] for number in range(4)]
            moved = cmul(here[0], here[1], real, imag)
            real, imag = moved[0] + here[2], moved[1] + here[3]
        factor_ref[...] = spread_keep(keep_ref[way], groups, states)

        def step(k, carry):
            real, imag = carry
            at = k if way == 0 else span - 1 - k
            rows = pl.ds(pl.multiple_of(at * CHUNKS, CHUNKS), CHUNKS)
            factor = factor_ref[rows]
            real, imag = factor * real, factor * imag
            real, imag = cmul(pole_real, pole_imag, real, imag)
            real = real + drive_ref[2 * way, rows]
            imag = imag + drive_ref[2 * way + 1, rows]
            real_ref[rows] = real
            imag_ref[rows] = imag
            return real, imag

        lax.fori_loop(0, span, step, (start_ref[0], start_ref[1]))
        for part, held in enumerate((real_ref, imag_ref)):
            high, low = split(held[...])
            read_high, read_low = split(read_ref[2 * way + part])
            wide_high = jnp.dot(read_high, tile, preferred_element_type=F32)
            wide_high = jnp.where(own, wide_high, 0.0).astype(BF)
            wide_low = jnp.dot(read_low, tile, preferred_element_type=F32)
            wide_low = jnp.where(own, wide_low, 0.0).astype(BF)
            y_ref[...] += (
                dot_nt(high, wide_high) + dot_nt(low, wide_high) + dot_nt(high, wide_low)
            )
    y = y_ref[...]
    inner = 0.7978845608028654 * (y + 0.044715 * (y * y * y))
    out_ref[...] = (0.5 * y * (1.0 + jnp.tanh(inner))).astype(BF)


def vmem(count):
    return [pl.BlockSpec(memory_space=pltpu.VMEM)] * count


def smem(count):
    return [pl.BlockSpec(memory_space=pltpu.SMEM)] * count


def interleave(array):
    tokens = array.shape[0]
    parts = array.reshape((CHUNKS, tokens // CHUNKS) + array.shape[1:])
    return jnp.swapaxes(parts, 0, 1).reshape(array.shape)


def deinterleave(array):
    tokens = array.shape[0]
    parts = array.reshape((tokens // CHUNKS, CHUNKS) + array.shape[1:])
    return jnp.swapaxes(parts, 0, 1).reshape(array.shape)


def mixing(
    mix_input, doc_ids, log_dt, decay_rate, frequency, input_real, input_imag,
    output_real, output_imag, skip_gain, log_keep,
):
    tokens, width = mix_input.shape
    groups, states = decay_rate.shape
    flat = groups * states
    pole_real, pole_imag, zoh_real, zoh_imag = discretize(log_dt, decay_rate, frequency)
    map_real, map_imag = input_maps(zoh_real, zoh_imag, input_real, input_imag)
    maps = jnp.stack([map_real, map_imag], 1).reshape(4, flat, GROUP)
    reads = jnp.stack([output_real, -output_imag], 1).reshape(4, width, states)
    poles = jnp.stack([pole_real.reshape(flat), pole_imag.reshape(flat)])
    same = (doc_ids[1:] == doc_ids[:-1]).astype(F32)
    one = jnp.ones((1,), F32)
    links = jnp.stack([jnp.concatenate([one, same]), jnp.concatenate([same, one])])
    keep = jnp.exp(log_keep).T[None] * links[:, :, None]
    keep = jnp.stack([interleave(keep[0]), interleave(keep[1])])
    u = interleave(mix_input)
    doc_edges = jnp.stack([doc_ids[0], doc_ids[-1]]).astype(F32)
    drive, chunk, total = pl.pallas_call(
        drive_kernel,
        out_shape=(
            jax.ShapeDtypeStruct((4, tokens, flat), F32),
            jax.ShapeDtypeStruct((2, 4, CHUNKS, flat), F32),
            jax.ShapeDtypeStruct((16, flat), F32),
        ),
        in_specs=vmem(4) + smem(1),
        out_specs=tuple(vmem(3)),
        scratch_shapes=[pltpu.VMEM((tokens, flat), F32)],
        compiler_params=pltpu.CompilerParams(vmem_limit_bytes=40 << 20),
        cost_estimate=pl.CostEstimate(flops=10**8, bytes_accessed=6 << 20, transcendentals=0),
        name="drive",
    )(u, keep, maps, poles, doc_edges)
    everything = lax.all_gather(total, "sp")
    devices = everything.shape[0]
    me = lax.axis_index("sp").astype(jnp.int32).reshape(1)
    mixed = pl.pallas_call(
        functools.partial(read_kernel, devices),
        out_shape=jax.ShapeDtypeStruct((tokens, width), BF),
        in_specs=vmem(8) + smem(2),
        out_specs=vmem(1)[0],
        scratch_shapes=[
            pltpu.VMEM((tokens, flat), F32),
            pltpu.VMEM((2, CHUNKS, flat), F32),
            pltpu.VMEM((tokens, flat), F32),
            pltpu.VMEM((tokens, flat), F32),
            pltpu.VMEM((tokens, width), F32),
        ],
        compiler_params=pltpu.CompilerParams(vmem_limit_bytes=40 << 20),
        cost_estimate=pl.CostEstimate(flops=10**8, bytes_accessed=6 << 20, transcendentals=0),
        name="read",
    )(u, keep, drive, chunk, everything, reads, poles, skip_gain[None], doc_edges, me)
    return deinterleave(mixed)


def shifted(weight, hop, ring):
    return lax.ppermute(weight, "sp", [(k, (k + hop) % ring) for k in range(ring)])


def rounded_sum(activations, weights, pieces):
    block_width = activations.shape[1] // pieces
    summed = jnp.zeros((activations.shape[0], weights.shape[1]), jnp.float32)
    for number in range(pieces):
        lower = number * block_width
        partial_value = jnp.dot(
            activations[:, lower : lower + block_width],
            weights[lower : lower + block_width],
            preferred_element_type=jnp.float32,
        ).astype(jnp.bfloat16)
        summed = summed + lax.optimization_barrier(partial_value).astype(jnp.float32)
    return summed


def local(
    mix_input,
    stream,
    doc_ids,
    log_dt,
    decay_rate,
    frequency,
    input_real,
    input_imag,
    output_real,
    output_imag,
    skip_gain,
    log_keep,
    proj_weight,
    norm_gain,
    gate_weight,
    up_weight,
    down_weight,
):
    ring, here = lax.axis_size("sp"), lax.axis_index("sp")
    gates, ups, downs = (
        [weight] + [shifted(weight, hop, ring) for hop in range(1, ring)]
        for weight in (gate_weight, up_weight, down_weight)
    )
    mixed = mixing(
        mix_input, doc_ids, log_dt, decay_rate, frequency, input_real, input_imag,
        output_real, output_imag, skip_gain, log_keep,
    )
    tp_size = lax.axis_size("tp")
    spread = lax.all_to_all(mixed, "tp", split_axis=0, concat_axis=1, tiled=True)
    proj_whole = lax.all_gather(proj_weight, "tp", axis=0, tiled=True)
    branch = rounded_sum(spread, proj_whole, tp_size)
    resid = stream.astype(jnp.float32) + branch
    scale = lax.rsqrt(jnp.mean(resid * resid, axis=-1, keepdims=True) + 1e-06)
    normed = (resid * scale * norm_gain).astype(jnp.bfloat16)
    rows_all = lax.all_gather(normed, "tp", axis=0, tiled=True)
    depth = gate_weight.shape[0]
    columns = down_weight.shape[1]
    gate = upward = None
    for hop in range(ring):
        owner = lax.rem(here - hop + ring, ring)
        rows = lax.dynamic_slice_in_dim(rows_all, owner * depth, depth, 1)
        part = jnp.dot(rows, gates[hop], preferred_element_type=jnp.float32)
        gate = part if gate is None else gate + part
        part = jnp.dot(rows, ups[hop], preferred_element_type=jnp.float32)
        upward = part if upward is None else upward + part
    hidden = (jax.nn.silu(gate) * upward).astype(jnp.bfloat16)
    partial_out = jnp.zeros((hidden.shape[0], ring * columns), jnp.bfloat16)
    for hop in range(ring):
        owner = lax.rem(here - hop + ring, ring)
        part = jnp.dot(hidden, downs[hop], preferred_element_type=jnp.float32)
        partial_out = lax.dynamic_update_slice_in_dim(
            partial_out, part.astype(jnp.bfloat16), owner * columns, 1
        )
    ffn = lax.psum_scatter(
        partial_out.astype(jnp.bfloat16), "tp", scatter_dimension=0, tiled=True
    ).astype(jnp.float32)
    return (resid + 0.5 * ffn).astype(jnp.bfloat16)


def solution(mesh):
    placed = (
        P("sp", "tp"),
        P(("sp", "tp"), None),
        P("sp"),
        P("tp"),
        P("tp", None),
        P("tp", None),
        P(None, "tp", None, None),
        P(None, "tp", None, None),
        P(None, "tp", None, None),
        P(None, "tp", None, None),
        P("tp"),
        P("tp", "sp"),
        P("tp", None),
        P(),
        P("sp", "tp"),
        P("sp", "tp"),
        P("tp", "sp"),
    )
    return jax.shard_map(
        local, mesh=mesh, in_specs=placed, out_specs=P(("sp", "tp"), None), check_vma=False
    )
```
